32 devices in a mesh: sp: 8 (over z, core), tp: 4 (over y, x).
Axes of the slice: x: 2, y: 2, z: 4, core: 2. Of those that a mesh axis runs over, the one named last changes fastest.
Arguments:
- tokens: bfloat16 [1536, 4096], P('sp', 'tp'), may hold values from -60 to 60
- lean_query: bfloat16 [1536, 16, 64], P('sp', 'tp'), may hold values from -6 to 6
- lean_key: bfloat16 [1536, 2, 64], P('sp'), may hold values from -6 to 6
- lean_value: bfloat16 [1536, 2, 64], P('sp'), may hold values from -6 to 6
- lean_gains: float32 [2, 64], replicated, may hold values from 0.25 to 7.5
- broad_query: bfloat16 [1536, 16, 128], P('sp', 'tp'), may hold values from -6 to 6
- broad_key: bfloat16 [1536, 2, 128], P('sp'), may hold values from -6 to 6
- broad_value: bfloat16 [1536, 2, 128], P('sp'), may hold values from -6 to 6
- broad_gains: float32 [2, 128], replicated, may hold values from 0.25 to 7.5
- mixer_gain: float32 [3072], replicated, may hold values from 0.1 to 1.9
- output_weight: bfloat16 [3072, 4096], P(None, 'tp'), may hold values from -0.109375 to 0.109375
- channel_gain: float32 [4096], P('tp'), may hold values from 0.1 to 1.9
- gate_weight: bfloat16 [8, 4096, 2048], P('sp', None, 'tp'), may hold values from -0.09375 to 0.09375
- up_weight: bfloat16 [8, 4096, 2048], P('sp', None, 'tp'), may hold values from -0.09375 to 0.09375
- down_weight: bfloat16 [8, 2048, 4096], P('sp', None, 'tp'), may hold values from -0.125 to 0.125
- route_experts: int32 [1536, 2], P('sp'), may hold values from 0 to 7, as said below
- route_logits: float32 [1536, 2], P('sp'), may hold values from -6 to 6
- group_weight: float32 [1536], P('sp'), may hold values from 0.3 to 1
Outputs:
- encoded: bfloat16 [1536, 4096], P('sp', 'tp')
The draws below stay inside these ranges and needn't reach their ends.
Inputs may be any that keep to these rules, and one draw needn't show every extreme that they name: `route_experts`: each row names two different experts of one group, expert e lying in group e // 2. In every aligned block of 192 rows no expert is named by more than 96 rows; one group, the same for all blocks, is named by exactly half of each block's rows, and each of its experts by exactly 96 of them.
All inputs are finite; a program needn't handle non-finite values.
Results may differ from the reference program's by a relative error of at most 0.0083.
Values may be sent and summed in bfloat16 or wider, within the bound.
No kernel may reach another device: no remote copies, remote signals or barrier semaphores. Data moves between devices by JAX's collectives and lax.ppermute only.
A program may use at most 64 MiB of HBM per device.

```python
import jax
import jax.numpy as jnp
from jax import lax

TOK_SP = 192
SEQ = 1536
D = 4096
HQ_A = 16
KV_A = 2
HD_A = 64
HQ_B = 16
KV_B = 2
HD_B = 128
DMIX = 3072
GRID_W = 64
EXPERTS = 8
GROUPS = 4
EPG = 2
TOPK = 2
FF = 2048
CAP = 96
N_SP = 8


def drawn_pair(base_key, head_count, key_heads, head_size):
    subkeys = jax.random.split(base_key, 2)
    keys = jax.random.normal(subkeys[0], (SEQ, key_heads, head_size), jnp.float32)
    queries = jax.random.normal(subkeys[1], (SEQ, head_count, head_size), jnp.float32)
    return (jnp.clip(queries, -6.0, 6.0), jnp.clip(keys, -6.0, 6.0))


def gain_draw(base_key, head_size):
    return 1.0 + 0.18 * jnp.clip(jax.random.normal(base_key, (2, head_size), jnp.float32), -4.0, 4.0)


def draw_lean_query(key, part):
    return drawn_pair(jax.random.fold_in(key, 101), HQ_A, KV_A, HD_A)[0].astype(jnp.bfloat16)


def draw_lean_key(key, part):
    return drawn_pair(jax.random.fold_in(key, 101), HQ_A, KV_A, HD_A)[1].astype(jnp.bfloat16)


def draw_broad_query(key, part):
    return drawn_pair(jax.random.fold_in(key, 102), HQ_B, KV_B, HD_B)[0].astype(jnp.bfloat16)


def draw_broad_key(key, part):
    return drawn_pair(jax.random.fold_in(key, 102), HQ_B, KV_B, HD_B)[1].astype(jnp.bfloat16)


def draw_lean_gains(key, part):
    return gain_draw(jax.random.fold_in(key, 201), HD_A)


def draw_broad_gains(key, part):
    return gain_draw(jax.random.fold_in(key, 202), HD_B)


def draw_tokens(key, part):
    first_key, second_key = jax.random.split(jax.random.fold_in(key, 401))
    column = jnp.arange(D, dtype=jnp.float32) / D
    base_values = jnp.clip(jax.random.normal(first_key, (SEQ, D), jnp.float32), -5.0, 5.0)
    column_scale = 0.3 * 10.0 ** column
    row_scale = 0.4 * 10.0 ** jax.random.uniform(second_key, (SEQ, 1), jnp.float32)
    return (base_values * column_scale[None, :] * row_scale).astype(jnp.bfloat16)


def draw_route_experts(key, part):
    block_count = SEQ // TOK_SP
    half_rows = TOK_SP // 2
    big_group = jax.random.randint(jax.random.fold_in(key, 7), (), 0, GROUPS)
    block_keys = jax.random.split(jax.random.fold_in(key, 11), block_count)

    def one_block(block_key):
        cut_key, order_key, rank_key, inner_key = jax.random.split(block_key, 4)
        cut_points = jnp.sort(jax.random.randint(cut_key, (GROUPS - 2,), 0, half_rows + 1))
        bounds = jnp.concatenate([jnp.zeros((1,), jnp.int32), cut_points, jnp.full((1,), half_rows, jnp.int32)])
        starts = jnp.concatenate([jnp.zeros((1,), jnp.int32), half_rows + bounds[:-1]])
        ends = jnp.concatenate([jnp.full((1,), half_rows, jnp.int32), half_rows + bounds[1:]])
        others = (big_group + 1 + jax.random.permutation(order_key, GROUPS - 1)) % GROUPS
        group_order = jnp.concatenate([big_group[None], others])
        token_rank = jax.random.permutation(rank_key, TOK_SP)
        member = ((token_rank[:, None] >= starts[None, :]) & (token_rank[:, None] < ends[None, :])).astype(jnp.int32)
        which = jnp.argmax(member, axis=1)
        chosen_group = group_order[which]
        inner = token_rank - starts[which]
        first_pick = inner % EPG
        second_pick = (inner + 1 + inner // EPG % (EPG - 1)) % EPG
        shuffles = jax.vmap(lambda each_key: jax.random.permutation(each_key, EPG))(jax.random.split(inner_key, GROUPS))
        first_expert = chosen_group * EPG + shuffles[chosen_group, first_pick]
        second_expert = chosen_group * EPG + shuffles[chosen_group, second_pick]
        return jnp.stack([first_expert, second_expert], axis=1)
    return jax.vmap(one_block)(block_keys).reshape(SEQ, TOPK).astype(jnp.int32)


def shard_levels(rng, dims, pieces, low, high):
    loudness = 1.0
    for position, parts in pieces:
        draws = jax.random.uniform(jax.random.fold_in(jax.random.fold_in(rng, 6), position), (parts,), jnp.float32, low / len(pieces), high / len(pieces))
        loudness = loudness * jnp.repeat(jnp.exp(draws), dims[position] // parts).reshape((-1,) + (1,) * (len(dims) - 1 - position))
    return loudness


def gaussian(own_key, dims, spread, limit, cuts=(), kind=jnp.bfloat16):
    values = spread * jax.random.normal(own_key, dims, jnp.float32)
    if cuts:
        values = values * shard_levels(own_key, dims, cuts, -0.22, 0.18)
    return jnp.clip(values, -limit, limit).astype(kind)


def setup_inputs(seed: int = 0) -> dict:
    splits = jax.random.split(jax.random.key(seed), 19)
    return {
        "tokens": draw_tokens(jax.random.fold_in(splits[18], 71), 0),
        "lean_query": draw_lean_query(jax.random.fold_in(splits[18], 71), 0),
        "lean_key": draw_lean_key(jax.random.fold_in(splits[18], 71), 0),
        "lean_value": gaussian(splits[3], (SEQ, KV_A, HD_A), 1.0, 6.0, ((0, 8),)),
        "lean_gains": draw_lean_gains(jax.random.fold_in(splits[18], 71), 0),
        "broad_query": draw_broad_query(jax.random.fold_in(splits[18], 71), 0),
        "broad_key": draw_broad_key(jax.random.fold_in(splits[18], 71), 0),
        "broad_value": gaussian(splits[7], (SEQ, KV_B, HD_B), 1.0, 6.0, ((0, 8),)),
        "broad_gains": draw_broad_gains(jax.random.fold_in(splits[18], 71), 0),
        "mixer_gain": jnp.clip(1.0 + 0.18 * jax.random.normal(splits[9], (DMIX,), jnp.float32), 0.1, 1.9),
        "output_weight": gaussian(splits[10], (DMIX, D), DMIX ** -0.5, 0.109375, ((1, 4),)),
        "channel_gain": jnp.clip(1.0 + 0.18 * jax.random.normal(splits[11], (D,), jnp.float32), 0.1, 1.9),
        "gate_weight": gaussian(splits[12], (EXPERTS, D, FF), D ** -0.5, 0.09375, ((0, 8), (2, 4))),
        "up_weight": gaussian(splits[13], (EXPERTS, D, FF), D ** -0.5, 0.09375, ((0, 8), (2, 4))),
        "down_weight": gaussian(splits[14], (EXPERTS, FF, D), FF ** -0.5, 0.125, ((0, 8), (2, 4))),
        "route_experts": draw_route_experts(jax.random.fold_in(splits[18], 71), 0),
        "route_logits": gaussian(splits[16], (SEQ, TOPK), 1.5, 6.0, ((0, 8),), jnp.float32),
        "group_weight": jnp.clip(0.3 + 0.7 * jax.random.uniform(splits[17], (SEQ,), jnp.float32) ** shard_levels(splits[17], (SEQ,), ((0, 8),), -0.2, 0.2), 0.3, 1.0),
    }


epsilon = 1e-06
theta_base = 10000.0

def axial_angles(positions, head_size):
    quarter = head_size // 4
    frequency = theta_base ** (-jnp.arange(quarter, dtype=jnp.float32) / quarter)
    grid_rows = (positions // GRID_W).astype(jnp.float32)
    grid_columns = (positions % GRID_W).astype(jnp.float32)
    return (grid_rows[:, None] * frequency[None, :], grid_columns[:, None] * frequency[None, :])

def turn_half(values, angles):
    half_width = values.shape[-1] // 2
    first_half = values[..., :half_width]
    second = values[..., half_width:]
    cosine = jnp.cos(angles)[:, None, :]
    sine_part = jnp.sin(angles)[:, None, :]
    return jnp.concatenate([first_half * cosine - second * sine_part, second * cosine + first_half * sine_part], axis=-1)

def prepare(raw_values, gain_row, positions):
    values = raw_values.astype(jnp.float32)
    values = values * lax.rsqrt(lax.optimization_barrier(jnp.mean(values * values, axis=-1, keepdims=True)) + epsilon) * gain_row
    row_angles, column_angles = axial_angles(positions, raw_values.shape[-1])
    half_width = raw_values.shape[-1] // 2
    turned = jnp.concatenate([turn_half(values[..., :half_width], row_angles), turn_half(values[..., half_width:], column_angles)], axis=-1)
    return turned.astype(jnp.bfloat16)

def attend(queries, keys, values):
    token_count, head_count, head_size = queries.shape
    key_heads = keys.shape[1]
    group_ratio = head_count // key_heads
    blocks = queries.reshape(token_count // TOK_SP, TOK_SP, key_heads, group_ratio, head_size)
    keys_wide = keys.astype(jnp.float32)
    values_wide = values.astype(jnp.float32)

    def one_block(block_queries):
        scores = jnp.einsum('qkgd,skd->kgqs', block_queries.astype(jnp.float32), keys_wide) * head_size ** (-0.5)
        peak_score = lax.optimization_barrier(jnp.max(scores, axis=-1, keepdims=True))
        weights = jnp.exp(scores - peak_score)
        weight_sum = lax.optimization_barrier(jnp.sum(weights, axis=-1))
        rounded = lax.optimization_barrier(weights.astype(jnp.bfloat16)).astype(jnp.float32)
        summed = jnp.einsum('kgqs,skd->qkgd', rounded, values_wide)
        return (summed / jnp.transpose(weight_sum, (2, 0, 1))[..., None]).astype(jnp.bfloat16)
    mixed_heads = lax.map(one_block, blocks)
    return mixed_heads.reshape(token_count, head_count * head_size)

def group_norm(head_rows, gain_row):
    values = head_rows.astype(jnp.float32)
    return (values * lax.rsqrt(lax.optimization_barrier(jnp.mean(values * values, axis=-1, keepdims=True)) + epsilon) * gain_row).astype(jnp.bfloat16)

def reference(tokens, lean_query, lean_key, lean_value, lean_gains, broad_query, broad_key, broad_value, broad_gains, mixer_gain, output_weight, channel_gain, gate_weight, up_weight, down_weight, route_experts, route_logits, group_weight):
    positions = jnp.arange(SEQ, dtype=jnp.int32)
    lean_out = attend(prepare(lean_query, lean_gains[0], positions), prepare(lean_key, lean_gains[1], positions), lean_value)
    broad_out = attend(prepare(broad_query, broad_gains[0], positions), prepare(broad_key, broad_gains[1], positions), broad_value)
    lean_width = HQ_A * HD_A
    mixed_rows = jnp.concatenate([group_norm(lean_out, mixer_gain[:lean_width]), group_norm(broad_out, mixer_gain[lean_width:])], axis=1)
    stream = tokens.astype(jnp.float32) + jnp.dot(mixed_rows, output_weight, preferred_element_type=jnp.float32)
    normed = (stream * lax.rsqrt(lax.optimization_barrier(jnp.mean(stream * stream, axis=-1, keepdims=True)) + epsilon) * channel_gain).astype(jnp.bfloat16)
    logit_gap = route_logits[:, 0] - route_logits[:, 1]
    weights = group_weight[:, None] * jax.nn.sigmoid(jnp.stack([logit_gap, -logit_gap], axis=1))
    row_bound = N_SP * CAP

    def one_expert(running, expert_index):
        hit_mask = route_experts == expert_index
        member = jnp.any(hit_mask, axis=1)
        chosen = jnp.nonzero(member, size=row_bound, fill_value=0)[0]
        valid_rows = (jnp.arange(row_bound) < jnp.sum(member.astype(jnp.int32))).astype(jnp.float32)
        picked = normed[chosen]
        gate_value = jnp.dot(picked, gate_weight[expert_index], preferred_element_type=jnp.float32)
        up_value = jnp.dot(picked, up_weight[expert_index], preferred_element_type=jnp.float32)
        hidden = (jax.nn.silu(gate_value) * up_value).astype(jnp.bfloat16)
        result = jnp.dot(hidden, down_weight[expert_index], preferred_element_type=jnp.float32).astype(jnp.bfloat16)
        coefficient = lax.optimization_barrier(jnp.sum(jnp.where(hit_mask, weights, 0.0), axis=1))[chosen] * valid_rows
        return (running.at[chosen].add(coefficient[:, None] * result.astype(jnp.float32)), None)
    routed = lax.scan(one_expert, jnp.zeros((SEQ, D), jnp.float32), jnp.arange(EXPERTS, dtype=jnp.int32))[0]
    return (stream + routed).astype(jnp.bfloat16)
```

```python
import jax
import jax.numpy as jnp
from jax import lax
from jax.sharding import PartitionSpec as P

D = 4096
HQ_A = 16
KV_A = 2
HQ_B = 16
KV_B = 2
GRID_W = 64
GROUPS = 4


epsilon = 1e-06
theta_base = 10000.0
floor_score = -1e30

PIECES = ((0,), (1, 2, 3))


def axial_angles(positions, head_size):
    quarter = head_size // 4
    frequency = theta_base ** (-jnp.arange(quarter, dtype=jnp.float32) / quarter)
    grid_rows = (positions // GRID_W).astype(jnp.float32)
    grid_columns = (positions % GRID_W).astype(jnp.float32)
    return (grid_rows[:, None] * frequency[None, :], grid_columns[:, None] * frequency[None, :])


def turn_half(values, angles):
    half_width = values.shape[-1] // 2
    first_half = values[..., :half_width]
    second = values[..., half_width:]
    cosine = jnp.cos(angles)[:, None, :]
    sine_part = jnp.sin(angles)[:, None, :]
    return jnp.concatenate(
        [first_half * cosine - second * sine_part, second * cosine + first_half * sine_part],
        axis=-1,
    )


def prepare(raw_values, gain_row, positions):
    values = raw_values.astype(jnp.float32)
    values = (
        values * lax.rsqrt(jnp.mean(values * values, axis=-1, keepdims=True) + epsilon) * gain_row
    )
    row_angles, column_angles = axial_angles(positions, raw_values.shape[-1])
    half_width = raw_values.shape[-1] // 2
    turned = jnp.concatenate(
        [
            turn_half(values[..., :half_width], row_angles),
            turn_half(values[..., half_width:], column_angles),
        ],
        axis=-1,
    )
    return turned.astype(jnp.bfloat16)


def group_norm(head_rows, gain_row):
    values = head_rows.astype(jnp.float32)
    return (
        values * lax.rsqrt(jnp.mean(values * values, axis=-1, keepdims=True) + epsilon) * gain_row
    ).astype(jnp.bfloat16)


def own_heads(query_raw, key_raw, value_raw, gain_pair, positions, lane_index, group_ratio):
    head_count, head_size = (query_raw.shape[1], query_raw.shape[2])
    key_heads = max(1, head_count // group_ratio)
    kv_start = lane_index * head_count // group_ratio
    key_part = lax.dynamic_slice_in_dim(key_raw, kv_start, key_heads, 1)
    value_part = lax.dynamic_slice_in_dim(value_raw, kv_start, key_heads, 1)
    queries = prepare(query_raw, gain_pair[0], positions).reshape(
        query_raw.shape[0], key_heads, head_count // key_heads, head_size
    )
    return (queries, prepare(key_part, gain_pair[1], positions), value_part)


def start_state(queries):
    row_count = queries.shape[0]
    head_count = queries.shape[1] * queries.shape[2]
    return (
        jnp.full((head_count, row_count), floor_score, jnp.float32),
        jnp.zeros((head_count, row_count), jnp.float32),
        jnp.zeros((row_count, head_count, queries.shape[3]), jnp.float32),
    )


def attend_piece(fold_state, queries, keys, values):
    peak_score, weight_sum, accumulated = fold_state
    row_count, key_heads, grouped, head_size = queries.shape
    key_count = keys.shape[0]
    scores = jnp.einsum(
        "qkgd,skd->kgqs", queries, keys, preferred_element_type=jnp.float32
    ) * head_size ** (-0.5)
    scores = scores.reshape(key_heads * grouped, row_count, key_count)
    new_peak = jnp.maximum(peak_score, jnp.max(scores, axis=-1))
    weights = jnp.exp(scores - new_peak[..., None])
    new_sum = jnp.sum(weights, axis=-1)
    rounded = weights.astype(jnp.bfloat16).reshape(key_heads, grouped, row_count, key_count)
    partial_value = jnp.einsum(
        "kgqs,skd->qkgd", rounded, values, preferred_element_type=jnp.float32
    )
    partial_value = partial_value.reshape(row_count, key_heads * grouped, head_size)
    return (new_peak, new_sum, partial_value)


def finish_heads(fold_state):
    accumulated = fold_state[2]
    return (
        (accumulated / jnp.transpose(fold_state[1])[:, :, None])
        .astype(jnp.bfloat16)
        .reshape(accumulated.shape[0], -1)
    )


def gather_pair(keys, values):
    rows, heads, size = keys.shape
    packed = jnp.concatenate([keys, values], axis=-1).reshape(rows, heads * 2 * size)
    packed = lax.all_gather(packed, "sp", axis=0, tiled=True).reshape(-1, heads, 2 * size)
    return (packed[..., :size], packed[..., size:])


def chip_shift(values, step):
    count = lax.axis_size("sp")
    return lax.ppermute(values, "sp", [(i, (i + 2 * step) % count) for i in range(count)])


def core_swap(values):
    return lax.ppermute(values, "sp", [(i, i ^ 1) for i in range(lax.axis_size("sp"))])


def lane_swap(values, mask):
    return lax.ppermute(values, "tp", [(i, i ^ mask) for i in range(lax.axis_size("tp"))])


def lane_spread(values):
    half = values.shape[0] // 2
    near = lane_swap(values, 1)
    far = lane_swap(values, 2)
    corner = jnp.concatenate([lane_swap(far[:half], 1), lane_swap(near[half:], 2)], axis=0)
    return (values, near, far, corner)


def lane_rows(weight):
    lane = lax.axis_index("tp")
    size = weight.shape[0] // lax.axis_size("tp")
    return [lax.dynamic_slice_in_dim(weight, (lane ^ m) * size, size, 0) for m in range(4)]


def split_dot(pieces, weights):
    return sum(jnp.dot(p, w, preferred_element_type=jnp.float32) for p, w in zip(pieces, weights))


def route_early(route_experts, route_logits, group_weight, channel_gain):
    rows = route_experts.shape[0]
    capacity = rows // 2
    here = lax.axis_index("sp") // 2
    core = lax.axis_index("sp") % 2
    group = route_experts[:, 0] // 2
    member = (group[:, None] == jnp.arange(GROUPS, dtype=jnp.int32)[None, :]).astype(jnp.float32)
    before = (jnp.arange(rows)[:, None] > jnp.arange(rows)[None, :]).astype(jnp.float32)
    rank = jnp.sum(jnp.dot(before, member) * member, axis=1).astype(jnp.int32)
    slot_of = jnp.mod(group - here, GROUPS) * capacity + rank
    slots = slot_of[None, :] == jnp.arange(GROUPS * capacity, dtype=jnp.int32)[:, None]
    gap = route_logits[:, 0] - route_logits[:, 1]
    weights = group_weight[:, None] * jax.nn.sigmoid(jnp.stack([gap, -gap], axis=1))
    by_core = [
        jnp.sum(jnp.where(route_experts % 2 == c, weights, 0.0), axis=1) for c in range(2)
    ]
    sent = jnp.stack(
        [jnp.sum(jnp.where(slots, w[None, :], 0.0), axis=1) for w in by_core]
    ).reshape(2, GROUPS, capacity)
    landed = jnp.stack([sent[:, 0]] + [chip_shift(sent[:, k], k) for k in range(1, GROUPS)])
    own = jnp.where(core == 0, landed[:, 0], landed[:, 1])
    other = core_swap(jnp.where(core == 0, landed[:, 1], landed[:, 0]))
    gain = channel_gain.reshape(8, -1)
    wide_gain = [channel_gain] + [lane_swap(gain, m).reshape(-1) for m in (1, 2, 3)]
    return (slots.astype(jnp.bfloat16), (own, other), wide_gain)


def experts_by_chip(stream, channel_gain, gate_part, up_part, down_part, slots, coefs, wide_gain):
    capacity = slots.shape[0] // GROUPS
    features = D
    scaled = (stream * channel_gain).astype(jnp.bfloat16)
    outgoing = jnp.dot(slots, scaled, preferred_element_type=jnp.float32).astype(jnp.bfloat16)
    outgoing = outgoing.reshape(GROUPS, capacity, -1)
    landed = [outgoing[0]] + [chip_shift(outgoing[k], k) for k in range(1, GROUPS)]
    gate_rows, up_rows, down_rows = lane_rows(gate_part), lane_rows(up_part), lane_rows(down_part)
    inverse = [(1.0 / (g * g))[None, :] for g in wide_gain]
    back = [None] * GROUPS
    for members in PIECES:
        own = lane_spread(jnp.concatenate([landed[k] for k in members], axis=0))
        pieces = [jnp.concatenate([p, core_swap(p)], axis=0) for p in own]
        squares = sum(
            jnp.sum(jnp.square(p.astype(jnp.float32)) * i, axis=1) for p, i in zip(pieces, inverse)
        )
        scale = lax.rsqrt(squares / features + epsilon)[:, None]
        gate_value = split_dot(pieces, gate_rows) * scale
        up_value = split_dot(pieces, up_rows) * scale
        hidden = (jax.nn.silu(gate_value) * up_value).astype(jnp.bfloat16)
        coef = jnp.concatenate([c[k] for c in coefs for k in members])[:, None]
        result = split_dot(lane_spread(hidden), down_rows) * coef
        rows = capacity * len(members)
        other = core_swap(result[rows:].astype(jnp.bfloat16)).astype(jnp.float32)
        total = (result[:rows] + other).astype(jnp.bfloat16).reshape(len(members), capacity, -1)
        for i, k in enumerate(members):
            back[k] = chip_shift(total[i], -k) if k else total[i]
    routed = lax.dot_general(
        slots,
        jnp.concatenate(back, axis=0),
        (((0,), (0,)), ((), ())),
        preferred_element_type=jnp.float32,
    )
    return (stream + routed).astype(jnp.bfloat16)


def on_device(
    tokens,
    lean_query,
    lean_key,
    lean_value,
    lean_gains,
    broad_query,
    broad_key,
    broad_value,
    broad_gains,
    mixer_gain,
    output_weight,
    channel_gain,
    gate_weight,
    up_weight,
    down_weight,
    route_experts,
    route_logits,
    group_weight,
):
    row_count = tokens.shape[0]
    positions = lax.axis_index("sp") * row_count + jnp.arange(row_count, dtype=jnp.int32)
    lane_index = lax.axis_index("tp")
    lean_queries, lean_keys, lean_values = own_heads(
        lean_query, lean_key, lean_value, lean_gains, positions, lane_index, HQ_A // KV_A
    )
    broad_queries, broad_keys, broad_values = own_heads(
        broad_query, broad_key, broad_value, broad_gains, positions, lane_index, HQ_B // KV_B
    )
    fast = lax.axis_size("tp") == 4 and lax.axis_size("sp") == 2 * GROUPS
    if fast:
        slots, coefs, wide_gain = route_early(route_experts, route_logits, group_weight, channel_gain)
    shard_rows = gather_pair(lean_keys, lean_values) + gather_pair(broad_keys, broad_values)
    lean_state = attend_piece(start_state(lean_queries), lean_queries, shard_rows[0], shard_rows[1])
    broad_state = attend_piece(
        start_state(broad_queries), broad_queries, shard_rows[2], shard_rows[3]
    )
    lean_all, broad_all = (
        lax.all_gather(finish_heads(lean_state), "tp", axis=1, tiled=True),
        lax.all_gather(finish_heads(broad_state), "tp", axis=1, tiled=True),
    )
    lean_width = lean_all.shape[1]
    stream = tokens.astype(jnp.float32) + jnp.dot(
        group_norm(lean_all, mixer_gain[:lean_width]),
        output_weight[:lean_width],
        preferred_element_type=jnp.float32,
    )
    stream = stream + jnp.dot(
        group_norm(broad_all, mixer_gain[lean_width:]),
        output_weight[lean_width:],
        preferred_element_type=jnp.float32,
    )
    if fast:
        return experts_by_chip(
            stream, channel_gain, gate_weight[0], up_weight[0], down_weight[0], slots, coefs, wide_gain
        )
    squares = lax.psum(jnp.sum(stream * stream, axis=1), "tp")
    normed = (stream * lax.rsqrt(squares / D + epsilon)[:, None] * channel_gain).astype(
        jnp.bfloat16
    )
    experts = lax.axis_size("sp")
    capacity = row_count // (experts // GROUPS)
    flat_experts = route_experts.reshape(-1)
    onehot = (flat_experts[:, None] == jnp.arange(experts, dtype=jnp.int32)[None, :]).astype(
        jnp.int32
    )
    slot_rank = jnp.sum((jnp.cumsum(onehot, axis=0) - 1) * onehot, axis=1)
    slot_index = flat_experts * capacity + slot_rank
    token_owner = jnp.repeat(jnp.arange(row_count, dtype=jnp.int32), route_experts.shape[1])
    filled = jnp.zeros((experts * capacity,), jnp.int32).at[slot_index].set(token_owner + 1)
    slot_live = (filled > 0)[:, None]
    source = jnp.maximum(filled - 1, 0)
    outgoing = jnp.where(slot_live, normed[source], jnp.zeros((), jnp.bfloat16)).reshape(
        experts, capacity, -1
    )
    arrived = lax.all_to_all(outgoing, "sp", split_axis=0, concat_axis=0, tiled=True)
    sources = arrived.shape[0]
    item_count = arrived.shape[1]
    shard_rows = lax.all_gather(arrived, "tp", axis=2, tiled=True)
    flat_rows = shard_rows.reshape(sources * item_count, shard_rows.shape[2])
    gate_part = gate_weight[0]
    up_part = up_weight[0]
    gate_value = jnp.dot(flat_rows, gate_part, preferred_element_type=jnp.float32)
    up_value = jnp.dot(flat_rows, up_part, preferred_element_type=jnp.float32)
    hidden = (jax.nn.silu(gate_value) * up_value).astype(jnp.bfloat16)
    down_part = down_weight[0]
    result = jnp.dot(
        lax.all_gather(hidden, "tp", axis=1, tiled=True),
        down_part,
        preferred_element_type=jnp.float32,
    )
    result = result.astype(jnp.bfloat16).reshape(sources, item_count, -1)
    returned = lax.all_to_all(result, "sp", split_axis=0, concat_axis=0, tiled=True)
    picked = (
        returned.reshape(experts * capacity, -1)[slot_index]
        .reshape(row_count, route_experts.shape[1], -1)
        .astype(jnp.float32)
    )
    logit_gap = route_logits[:, 0] - route_logits[:, 1]
    weights = group_weight[:, None] * jax.nn.sigmoid(jnp.stack([logit_gap, -logit_gap], axis=1))
    return (stream + jnp.sum(picked * weights[:, :, None], axis=1)).astype(jnp.bfloat16)


def solution(mesh):
    return jax.shard_map(
        on_device,
        mesh=mesh,
        in_specs=(
            P("sp", "tp"),
            P("sp", "tp", None),
            P("sp", None, None),
            P("sp", None, None),
            P(),
            P("sp", "tp", None),
            P("sp", None, None),
            P("sp", None, None),
            P(),
            P(),
            P(None, "tp"),
            P("tp"),
            P("sp", None, "tp"),
            P("sp", None, "tp"),
            P("sp", None, "tp"),
            P("sp", None),
            P("sp", None),
            P("sp"),
        ),
        out_specs=P("sp", "tp"),
        check_vma=False,
    )
```

```python
import jax
import jax.numpy as jnp
from jax import lax
from jax.sharding import PartitionSpec as P

D = 4096
HQ_A = 16
KV_A = 2
HQ_B = 16
KV_B = 2
GRID_W = 64
GROUPS = 4


epsilon = 1e-06
theta_base = 10000.0
floor_score = -1e30

PIECES = ((0, 2), (1, 3))


def axial_angles(positions, head_size):
    quarter = head_size // 4
    frequency = theta_base ** (-jnp.arange(quarter, dtype=jnp.float32) / quarter)
    grid_rows = (positions // GRID_W).astype(jnp.float32)
    grid_columns = (positions % GRID_W).astype(jnp.float32)
    return (grid_rows[:, None] * frequency[None, :], grid_columns[:, None] * frequency[None, :])


def turn_half(values, angles):
    half_width = values.shape[-1] // 2
    first_half = values[..., :half_width]
    second = values[..., half_width:]
    cosine = jnp.cos(angles)[:, None, :]
    sine_part = jnp.sin(angles)[:, None, :]
    return jnp.concatenate(
        [first_half * cosine - second * sine_part, second * cosine + first_half * sine_part],
        axis=-1,
    )


def prepare(raw_values, gain_row, positions):
    values = raw_values.astype(jnp.float32)
    values = (
        values * lax.rsqrt(jnp.mean(values * values, axis=-1, keepdims=True) + epsilon) * gain_row
    )
    row_angles, column_angles = axial_angles(positions, raw_values.shape[-1])
    half_width = raw_values.shape[-1] // 2
    turned = jnp.concatenate(
        [
            turn_half(values[..., :half_width], row_angles),
            turn_half(values[..., half_width:], column_angles),
        ],
        axis=-1,
    )
    return turned.astype(jnp.bfloat16)


def group_norm(head_rows, gain_row):
    values = head_rows.astype(jnp.float32)
    return (
        values * lax.rsqrt(jnp.mean(values * values, axis=-1, keepdims=True) + epsilon) * gain_row
    ).astype(jnp.bfloat16)


def own_heads(query_raw, key_raw, value_raw, gain_pair, positions, lane_index, group_ratio):
    head_count, head_size = (query_raw.shape[1], query_raw.shape[2])
    key_heads = max(1, head_count // group_ratio)
    kv_start = lane_index * head_count // group_ratio
    key_part = lax.dynamic_slice_in_dim(key_raw, kv_start, key_heads, 1)
    value_part = lax.dynamic_slice_in_dim(value_raw, kv_start, key_heads, 1)
    queries = prepare(query_raw, gain_pair[0], positions).reshape(
        query_raw.shape[0], key_heads, head_count // key_heads, head_size
    )
    return (queries, prepare(key_part, gain_pair[1], positions), value_part)


def start_state(queries):
    row_count = queries.shape[0]
    head_count = queries.shape[1] * queries.shape[2]
    return (
        jnp.full((head_count, row_count), floor_score, jnp.float32),
        jnp.zeros((head_count, row_count), jnp.float32),
        jnp.zeros((row_count, head_count, queries.shape[3]), jnp.float32),
    )


def attend_piece(fold_state, queries, keys, values):
    peak_score, weight_sum, accumulated = fold_state
    row_count, key_heads, grouped, head_size = queries.shape
    key_count = keys.shape[0]
    scores = jnp.einsum(
        "qkgd,skd->kgqs", queries, keys, preferred_element_type=jnp.float32
    ) * head_size ** (-0.5)
    scores = scores.reshape(key_heads * grouped, row_count, key_count)
    new_peak = jnp.maximum(peak_score, jnp.max(scores, axis=-1))
    weights = jnp.exp(scores - new_peak[..., None])
    new_sum = jnp.sum(weights, axis=-1)
    rounded = weights.astype(jnp.bfloat16).reshape(key_heads, grouped, row_count, key_count)
    partial_value = jnp.einsum(
        "kgqs,skd->qkgd", rounded, values, preferred_element_type=jnp.float32
    )
    partial_value = partial_value.reshape(row_count, key_heads * grouped, head_size)
    return (new_peak, new_sum, partial_value)


def finish_heads(fold_state):
    accumulated = fold_state[2]
    return (
        (accumulated / jnp.transpose(fold_state[1])[:, :, None])
        .astype(jnp.bfloat16)
        .reshape(accumulated.shape[0], -1)
    )


def gather_pair(keys, values):
    rows, heads, size = keys.shape
    packed = jnp.concatenate([keys, values], axis=-1).reshape(rows, heads * 2 * size)
    packed = lax.all_gather(packed, "sp", axis=0, tiled=True).reshape(-1, heads, 2 * size)
    return (packed[..., :size], packed[..., size:])


def chip_shift(values, step):
    count = lax.axis_size("sp")
    return lax.ppermute(values, "sp", [(i, (i + 2 * step) % count) for i in range(count)])


def core_swap(values):
    return lax.ppermute(values, "sp", [(i, i ^ 1) for i in range(lax.axis_size("sp"))])


def lane_swap(values, mask):
    return lax.ppermute(values, "tp", [(i, i ^ mask) for i in range(lax.axis_size("tp"))])


def lane_spread(values):
    half = values.shape[0] // 2
    near = lane_swap(values, 1)
    far = lane_swap(values, 2)
    corner = jnp.concatenate([lane_swap(far[:half], 1), lane_swap(near[half:], 2)], axis=0)
    return (values, near, far, corner)


def lane_rows(weight):
    lane = lax.axis_index("tp")
    size = weight.shape[0] // lax.axis_size("tp")
    return [lax.dynamic_slice_in_dim(weight, (lane ^ m) * size, size, 0) for m in range(4)]


def split_dot(pieces, weights):
    return sum(jnp.dot(p, w, preferred_element_type=jnp.float32) for p, w in zip(pieces, weights))


def mixed_dot(heads, gain, weight):
    pieces = [heads] + [lane_swap(heads, m) for m in (1, 2, 3)]
    wide = [p.astype(jnp.float32) for p in pieces]
    squares = sum(jnp.sum(v * v, axis=1, keepdims=True) for v in wide)
    scale = lax.rsqrt(squares / gain.shape[0] + epsilon)
    mixed = [(v * scale * g).astype(jnp.bfloat16) for v, g in zip(wide, lane_rows(gain))]
    return split_dot(mixed, lane_rows(weight))


def route_early(route_experts, route_logits, group_weight, channel_gain):
    rows = route_experts.shape[0]
    capacity = rows // 2
    here = lax.axis_index("sp") // 2
    core = lax.axis_index("sp") % 2
    group = route_experts[:, 0] // 2
    member = (group[:, None] == jnp.arange(GROUPS, dtype=jnp.int32)[None, :]).astype(jnp.float32)
    before = (jnp.arange(rows)[:, None] > jnp.arange(rows)[None, :]).astype(jnp.float32)
    rank = jnp.sum(jnp.dot(before, member) * member, axis=1).astype(jnp.int32)
    slot_of = jnp.mod(group - here, GROUPS) * capacity + rank
    slots = slot_of[None, :] == jnp.arange(GROUPS * capacity, dtype=jnp.int32)[:, None]
    gap = route_logits[:, 0] - route_logits[:, 1]
    weights = group_weight[:, None] * jax.nn.sigmoid(jnp.stack([gap, -gap], axis=1))
    by_core = [
        jnp.sum(jnp.where(route_experts % 2 == c, weights, 0.0), axis=1) for c in range(2)
    ]
    sent = jnp.stack(
        [jnp.sum(jnp.where(slots, w[None, :], 0.0), axis=1) for w in by_core]
    ).reshape(2, GROUPS, capacity)
    landed = jnp.stack([sent[:, 0]] + [chip_shift(sent[:, k], k) for k in range(1, GROUPS)])
    own = jnp.where(core == 0, landed[:, 0], landed[:, 1])
    other = core_swap(jnp.where(core == 0, landed[:, 1], landed[:, 0]))
    gain = channel_gain.reshape(8, -1)
    wide_gain = [channel_gain] + [lane_swap(gain, m).reshape(-1) for m in (1, 2, 3)]
    return (slots.astype(jnp.bfloat16), (own, other), wide_gain)


def experts_by_chip(stream, channel_gain, gate_part, up_part, down_part, slots, coefs, wide_gain):
    capacity = slots.shape[0] // GROUPS
    features = D
    scaled = (stream * channel_gain).astype(jnp.bfloat16)
    outgoing = jnp.dot(slots, scaled, preferred_element_type=jnp.float32).astype(jnp.bfloat16)
    outgoing = outgoing.reshape(GROUPS, capacity, -1)
    landed = [outgoing[0]] + [chip_shift(outgoing[k], k) for k in range(1, GROUPS)]
    gate_rows, up_rows, down_rows = lane_rows(gate_part), lane_rows(up_part), lane_rows(down_part)
    inverse = [(1.0 / (g * g))[None, :] for g in wide_gain]
    back = [None] * GROUPS
    for members in PIECES:
        own = lane_spread(jnp.concatenate([landed[k] for k in members], axis=0))
        pieces = [jnp.concatenate([p, core_swap(p)], axis=0) for p in own]
        squares = sum(
            jnp.sum(jnp.square(p.astype(jnp.float32)) * i, axis=1) for p, i in zip(pieces, inverse)
        )
        scale = lax.rsqrt(squares / features + epsilon)[:, None]
        gate_value = split_dot(pieces, gate_rows) * scale
        up_value = split_dot(pieces, up_rows) * scale
        hidden = (jax.nn.silu(gate_value) * up_value).astype(jnp.bfloat16)
        coef = jnp.concatenate([c[k] for c in coefs for k in members])[:, None]
        result = split_dot(lane_spread(hidden), down_rows) * coef
        rows = capacity * len(members)
        other = core_swap(result[rows:].astype(jnp.bfloat16)).astype(jnp.float32)
        total = (result[:rows] + other).astype(jnp.bfloat16).reshape(len(members), capacity, -1)
        for i, k in enumerate(members):
            back[k] = chip_shift(total[i], -k) if k else total[i]
    routed = lax.dot_general(
        slots,
        jnp.concatenate(back, axis=0),
        (((0,), (0,)), ((), ())),
        preferred_element_type=jnp.float32,
    )
    return (stream + routed).astype(jnp.bfloat16)


def on_device(
    tokens,
    lean_query,
    lean_key,
    lean_value,
    lean_gains,
    broad_query,
    broad_key,
    broad_value,
    broad_gains,
    mixer_gain,
    output_weight,
    channel_gain,
    gate_weight,
    up_weight,
    down_weight,
    route_experts,
    route_logits,
    group_weight,
):
    row_count = tokens.shape[0]
    positions = lax.axis_index("sp") * row_count + jnp.arange(row_count, dtype=jnp.int32)
    lane_index = lax.axis_index("tp")
    lean_queries, lean_keys, lean_values = own_heads(
        lean_query, lean_key, lean_value, lean_gains, positions, lane_index, HQ_A // KV_A
    )
    broad_queries, broad_keys, broad_values = own_heads(
        broad_query, broad_key, broad_value, broad_gains, positions, lane_index, HQ_B // KV_B
    )
    fast = lax.axis_size("tp") == 4 and lax.axis_size("sp") == 2 * GROUPS
    if fast:
        slots, coefs, wide_gain = route_early(route_experts, route_logits, group_weight, channel_gain)
    shard_rows = gather_pair(lean_keys, lean_values) + gather_pair(broad_keys, broad_values)
    lean_state = attend_piece(start_state(lean_queries), lean_queries, shard_rows[0], shard_rows[1])
    broad_state = attend_piece(
        start_state(broad_queries), broad_queries, shard_rows[2], shard_rows[3]
    )
    if fast:
        lean_width = lean_query.shape[1] * lean_query.shape[2] * lax.axis_size("tp")
        stream = tokens.astype(jnp.float32)
        stream = stream + mixed_dot(
            finish_heads(lean_state), mixer_gain[:lean_width], output_weight[:lean_width]
        )
        stream = stream + mixed_dot(
            finish_heads(broad_state), mixer_gain[lean_width:], output_weight[lean_width:]
        )
    else:
        lean_all, broad_all = (
            lax.all_gather(finish_heads(lean_state), "tp", axis=1, tiled=True),
            lax.all_gather(finish_heads(broad_state), "tp", axis=1, tiled=True),
        )
        lean_width = lean_all.shape[1]
        stream = tokens.astype(jnp.float32) + jnp.dot(
            group_norm(lean_all, mixer_gain[:lean_width]),
            output_weight[:lean_width],
            preferred_element_type=jnp.float32,
        )
        stream = stream + jnp.dot(
            group_norm(broad_all, mixer_gain[lean_width:]),
            output_weight[lean_width:],
            preferred_element_type=jnp.float32,
        )
    if fast:
        return experts_by_chip(
            stream, channel_gain, gate_weight[0], up_weight[0], down_weight[0], slots, coefs, wide_gain
        )
    squares = lax.psum(jnp.sum(stream * stream, axis=1), "tp")
    normed = (stream * lax.rsqrt(squares / D + epsilon)[:, None] * channel_gain).astype(
        jnp.bfloat16
    )
    experts = lax.axis_size("sp")
    capacity = row_count // (experts // GROUPS)
    flat_experts = route_experts.reshape(-1)
    onehot = (flat_experts[:, None] == jnp.arange(experts, dtype=jnp.int32)[None, :]).astype(
        jnp.int32
    )
    slot_rank = jnp.sum((jnp.cumsum(onehot, axis=0) - 1) * onehot, axis=1)
    slot_index = flat_experts * capacity + slot_rank
    token_owner = jnp.repeat(jnp.arange(row_count, dtype=jnp.int32), route_experts.shape[1])
    filled = jnp.zeros((experts * capacity,), jnp.int32).at[slot_index].set(token_owner + 1)
    slot_live = (filled > 0)[:, None]
    source = jnp.maximum(filled - 1, 0)
    outgoing = jnp.where(slot_live, normed[source], jnp.zeros((), jnp.bfloat16)).reshape(
        experts, capacity, -1
    )
    arrived = lax.all_to_all(outgoing, "sp", split_axis=0, concat_axis=0, tiled=True)
    sources = arrived.shape[0]
    item_count = arrived.shape[1]
    shard_rows = lax.all_gather(arrived, "tp", axis=2, tiled=True)
    flat_rows = shard_rows.reshape(sources * item_count, shard_rows.shape[2])
    gate_part = gate_weight[0]
    up_part = up_weight[0]
    gate_value = jnp.dot(flat_rows, gate_part, preferred_element_type=jnp.float32)
    up_value = jnp.dot(flat_rows, up_part, preferred_element_type=jnp.float32)
    hidden = (jax.nn.silu(gate_value) * up_value).astype(jnp.bfloat16)
    down_part = down_weight[0]
    result = jnp.dot(
        lax.all_gather(hidden, "tp", axis=1, tiled=True),
        down_part,
        preferred_element_type=jnp.float32,
    )
    result = result.astype(jnp.bfloat16).reshape(sources, item_count, -1)
    returned = lax.all_to_all(result, "sp", split_axis=0, concat_axis=0, tiled=True)
    picked = (
        returned.reshape(experts * capacity, -1)[slot_index]
        .reshape(row_count, route_experts.shape[1], -1)
        .astype(jnp.float32)
    )
    logit_gap = route_logits[:, 0] - route_logits[:, 1]
    weights = group_weight[:, None] * jax.nn.sigmoid(jnp.stack([logit_gap, -logit_gap], axis=1))
    return (stream + jnp.sum(picked * weights[:, :, None], axis=1)).astype(jnp.bfloat16)


def solution(mesh):
    return jax.shard_map(
        on_device,
        mesh=mesh,
        in_specs=(
            P("sp", "tp"),
            P("sp", "tp", None),
            P("sp", None, None),
            P("sp", None, None),
            P(),
            P("sp", "tp", None),
            P("sp", None, None),
            P("sp", None, None),
            P(),
            P(),
            P(None, "tp"),
            P("tp"),
            P("sp", None, "tp"),
            P("sp", None, "tp"),
            P("sp", None, "tp"),
            P("sp", None),
            P("sp", None),
            P("sp"),
        ),
        out_specs=P("sp", "tp"),
        check_vma=False,
    )
```
